256 devices in a mesh: sp: 32 (over z, y), tp: 8 (over x, core).
Axes of the slice: x: 4, y: 4, z: 8, core: 2. Of those that a mesh axis runs over, the one named last changes fastest.
Arguments:
- tokens: bfloat16 [4, 16384, 2048], P(None, ('sp', 'tp')), may hold values from -6 to 6
- in_gain: float32 [2048], replicated, may hold values from 0.1 to 1.9
- query_weight: bfloat16 [2048, 1024], P(None, 'tp'), may hold values from -0.125 to 0.125
- key_weight: bfloat16 [2048, 1024], P(None, 'tp'), may hold values from -0.125 to 0.125
- value_weight: bfloat16 [2048, 1024], P(None, 'tp'), may hold values from -0.125 to 0.125
- gate_weight: bfloat16 [2048, 1024], P(None, 'tp'), may hold values from -0.125 to 0.125
- log_decay: float32 [8], P('tp'), may hold values from -0.034 to 0, as said below
- norm_gain: float32 [1024], P('tp'), may hold values from 0.1 to 1.9
- out_weight: bfloat16 [1024, 2048], replicated, may hold values from -0.1875 to 0.1875
- post_gain: float32 [2048], replicated, may hold values from 0.1 to 1.9
Outputs:
- mixed: bfloat16 [4, 16384, 2048], P(None, ('sp', 'tp'))
The draws below stay inside these ranges and needn't reach their ends.
Inputs may be any that keep to these rules, and one draw needn't show every extreme that they name: `log_decay`: every entry is negative; some heads keep a tenth or more of their memory over 16384 positions, others lose most of it within 30 to 100 positions.
All inputs are finite; a program needn't handle non-finite values.
Results may differ from the reference program's by a relative error of at most 0.015.
Values may be sent and summed in bfloat16 or wider, within the bound.
No kernel may reach another device: no remote copies, remote signals or barrier semaphores. Data moves between devices by JAX's collectives and lax.ppermute only.
A program may use at most 64 MiB of HBM per device.

```python
import math
import jax
import jax.numpy as jnp
from jax import lax

D = 2048
HEADS = 8
HEAD_DIM = 128
BLOCK = 128
SEQS = 4
RET_WIDTH = 1024
SEQLEN = 16384


def draw_log_decay(key, part):
    head_order = jax.random.permutation(jax.random.fold_in(key, 11), HEADS)
    slow_heads = head_order < HEADS // 2
    uniform_draw = jax.random.uniform(jax.random.fold_in(key, 12), (HEADS,), jnp.float32)
    slow_rate = math.log(10.0) / SEQLEN * (0.1 + 0.9 * uniform_draw)
    fast_rate = jnp.exp(math.log(1.0 / 100.0) + uniform_draw * (math.log(1.0 / 30.0) - math.log(1.0 / 100.0)))
    return -jnp.where(slow_heads, slow_rate, fast_rate).astype(jnp.float32)


def level_of(stream_key, dims, pieces, smallest, high):
    level = 1.0
    for position, parts in pieces:
        steps = jax.random.uniform(jax.random.fold_in(jax.random.fold_in(stream_key, 6), position), (parts,), jnp.float32, smallest / len(pieces), high / len(pieces))
        level = level * jnp.repeat(jnp.exp(steps), dims[position] // parts).reshape((-1,) + (1,) * (len(dims) - 1 - position))
    return level


def noise(own_key, shape, scale, reach, split=(), kind=jnp.bfloat16):
    level = level_of(own_key, shape, split, -0.22, 0.18) if split else 1.0
    values = jax.random.normal(own_key, shape, jnp.float32) * scale * level
    return jnp.minimum(jnp.maximum(values, -reach), reach).astype(kind)


def setup_inputs(seed: int = 0) -> dict:
    keys = jax.random.split(jax.random.key(seed), 11)
    return {
        "tokens": noise(keys[0], (SEQS, SEQLEN, D), 1.0, 6.0, ((1, 256),)),
        "in_gain": jnp.clip(1.0 + 0.18 * jax.random.normal(keys[1], (D,), jnp.float32), 0.1, 1.9),
        "query_weight": noise(keys[2], (D, RET_WIDTH), D ** -0.5, 0.125, ((1, 8),)),
        "key_weight": noise(keys[3], (D, RET_WIDTH), D ** -0.5, 0.125, ((1, 8),)),
        "value_weight": noise(keys[4], (D, RET_WIDTH), D ** -0.5, 0.125, ((1, 8),)),
        "gate_weight": noise(keys[5], (D, RET_WIDTH), D ** -0.5, 0.125, ((1, 8),)),
        "log_decay": draw_log_decay(jax.random.fold_in(keys[10], 71), 0),
        "norm_gain": jnp.clip(1.0 + 0.18 * jax.random.normal(keys[7], (RET_WIDTH,), jnp.float32), 0.1, 1.9),
        "out_weight": noise(keys[8], (RET_WIDTH, D), RET_WIDTH ** -0.5, 0.1875),
        "post_gain": jnp.clip(1.0 + 0.18 * jax.random.normal(keys[9], (D,), jnp.float32), 0.1, 1.9),
    }


rms_eps = 1e-06
group_eps = 1e-05
rope_base = 10000.0
highest = lax.Precision.HIGHEST

def rotate(values, positions):
    half_dim = values.shape[-1] // 2
    inverse = rope_base ** (-jnp.arange(half_dim, dtype=jnp.float32) / half_dim)
    angles = positions.astype(jnp.float32)[:, None] * inverse[None, :]
    cosine = jnp.cos(angles)
    sine_part = jnp.sin(angles)
    first_half = values[..., :half_dim].astype(jnp.float32)
    second = values[..., half_dim:].astype(jnp.float32)
    return jnp.concatenate([first_half * cosine - second * sine_part, first_half * sine_part + second * cosine], axis=-1)

def retain(queries, key_rows, values, log_decay):
    seq_count, head_count, length, head_width = queries.shape
    block_count = length // BLOCK
    offsets = jnp.arange(BLOCK, dtype=jnp.float32)
    distance = offsets[:, None] - offsets[None, :]
    rate_col = log_decay[:, None, None]
    inside = jnp.where(distance >= 0, jnp.exp(rate_col * jnp.maximum(distance, 0.0)), 0.0)
    query_scale = jnp.exp(log_decay[:, None] * (offsets + 1.0))[..., None]
    key_scale = jnp.exp(log_decay[:, None] * (BLOCK - 1.0 - offsets))[..., None]
    block_decay = jnp.exp(log_decay * BLOCK)[:, None, None]

    def to_blocks(arr):
        return arr.reshape(seq_count, head_count, block_count, BLOCK, arr.shape[-1]).transpose(2, 0, 1, 3, 4)

    def advance(memory, inputs):
        q_block, k_block, v_block = inputs
        qf = q_block.astype(jnp.float32)
        kf = k_block.astype(jnp.float32)
        vf = v_block.astype(jnp.float32)
        scores = jnp.einsum('shqd,shkd->shqk', qf, kf, precision=highest)
        weights = (scores * inside).astype(jnp.bfloat16)
        within = jnp.einsum('shqk,shkv->shqv', weights.astype(jnp.float32), vf, precision=highest)
        carried = jnp.einsum('shqd,shdv->shqv', qf * query_scale, memory, precision=highest)
        k_scaled = (kf * key_scale).astype(jnp.bfloat16)
        memory = memory * block_decay + jnp.einsum('shkd,shkv->shdv', k_scaled.astype(jnp.float32), vf, precision=highest)
        return (memory, within + carried)
    start_memory = jnp.zeros((seq_count, head_count, head_width, values.shape[-1]), jnp.float32)
    outputs = lax.scan(advance, start_memory, (to_blocks(queries), to_blocks(key_rows), to_blocks(values)))[1]
    return outputs.transpose(1, 2, 0, 3, 4).reshape(seq_count, head_count, length, values.shape[-1])

def reference(tokens, in_gain, query_weight, key_weight, value_weight, gate_weight, log_decay, norm_gain, out_weight, post_gain):
    seq_count, length, model_width = tokens.shape
    tok_f32 = tokens.astype(jnp.float32)
    normed = (tok_f32 * lax.rsqrt(lax.optimization_barrier(jnp.mean(tok_f32 * tok_f32, axis=-1, keepdims=True)) + rms_eps) * in_gain).astype(jnp.bfloat16)
    flat_rows = normed.reshape(seq_count * length, model_width)

    def project(weight_mat):
        result = jnp.dot(flat_rows, weight_mat, preferred_element_type=jnp.float32).astype(jnp.bfloat16)
        return result.reshape(seq_count, length, HEADS, HEAD_DIM).transpose(0, 2, 1, 3)
    positions = jnp.arange(length, dtype=jnp.int32)
    queries = rotate(project(query_weight), positions).astype(jnp.bfloat16)
    key_rows = (rotate(project(key_weight), positions) * HEAD_DIM ** (-0.5)).astype(jnp.bfloat16)
    values = project(value_weight)
    gating = jnp.dot(flat_rows, gate_weight, preferred_element_type=jnp.float32).astype(jnp.bfloat16)
    gating = gating.reshape(seq_count, length, RET_WIDTH)
    retained = retain(queries, key_rows, values, log_decay)
    center = lax.optimization_barrier(jnp.mean(retained, axis=-1, keepdims=True))
    spread = lax.optimization_barrier(jnp.mean(jnp.square(retained - center), axis=-1, keepdims=True))
    normal = ((retained - center) * lax.rsqrt(spread + group_eps)).transpose(0, 2, 1, 3).reshape(seq_count, length, RET_WIDTH)
    gated = (normal * norm_gain * jax.nn.silu(gating.astype(jnp.float32))).astype(jnp.bfloat16)
    premix = jnp.dot(gated.reshape(seq_count * length, RET_WIDTH), out_weight, preferred_element_type=jnp.float32)
    mixed = premix * lax.rsqrt(lax.optimization_barrier(jnp.mean(premix * premix, axis=-1, keepdims=True)) + rms_eps) * post_gain
    return mixed.astype(jnp.bfloat16).reshape(seq_count, length, model_width)
```

```python
import functools

import jax
import jax.numpy as jnp
from jax import lax
from jax.experimental import pallas as pl
from jax.experimental.pallas import tpu as pltpu
from jax.sharding import Mesh
from jax.sharding import PartitionSpec as P


HD = 128
SP_TP = ("z", "y", "x", "c")
NX, NY, NZ = 4, 4, 8
ROWS = 64
STRETCH = 512
rms_eps = 1e-06
group_eps = 1e-05
rope_base = 10000.0
F32 = jnp.float32
BF16 = jnp.bfloat16

OWN, PART, LEFT, LEFT_O, RIGHT, RIGHT_O, FAR, FAR_O = range(8)
A, B = 0, 1
GROUPS = (
    ((A, OWN), (B, OWN), (A, PART), (B, PART)),
    ((A, LEFT), (B, RIGHT), (A, LEFT_O), (B, RIGHT_O)),
    ((B, LEFT), (A, RIGHT), (B, LEFT_O), (A, RIGHT_O)),
    ((A, FAR), (B, FAR)),
    ((A, FAR_O), (B, FAR_O)),
)
PLACE = {}
for gi, group in enumerate(GROUPS):
    for pi, (half, chunk) in enumerate(group):
        for j in range(2):
            PLACE[(2 * half + j, chunk)] = (gi, pi, j)

VM = pl.BlockSpec(memory_space=pltpu.VMEM)
SM = pl.BlockSpec(memory_space=pltpu.SMEM)


def call(kernel, outs, ins, flops=0, name=None, smem=(), limit=None):
    specs = [SM if i in smem else VM for i in range(len(ins))]
    return pl.pallas_call(
        kernel,
        out_shape=outs,
        in_specs=specs,
        out_specs=jax.tree.map(lambda _: VM, outs),
        cost_estimate=pl.CostEstimate(flops=max(flops, 1), bytes_accessed=1 << 20, transcendentals=0),
        compiler_params=pltpu.CompilerParams(vmem_limit_bytes=limit) if limit else None,
        name=name,
    )(*ins)


def sds(shape, dtype):
    return jax.ShapeDtypeStruct(shape, dtype)


def norm_kernel(tok, gain, out_a, out_b):
    for s in range(4):
        x = tok[s].astype(F32)
        scale = lax.rsqrt(jnp.mean(x * x, axis=-1, keepdims=True) + rms_eps)
        (out_a if s < 2 else out_b)[s % 2] = (x * scale * gain[...]).astype(BF16)


def proj_kernel(group, first, last, refs):
    n = len(group)
    pos = 0
    idx, refs = (refs[0], refs[1:]) if last else (None, refs)
    pieces, refs = refs[:n], refs[n:]
    wq, wk, wv, wg, cos, sin, qdec, kdec = refs[:8]
    refs = refs[8:]
    if not first:
        s_in, refs = refs[0], refs[1:]
    out, refs = refs[0], refs[1:]
    rows = jnp.concatenate([p[...].reshape(2 * ROWS, p.shape[-1]) for p in pieces], axis=0)
    joined = jnp.concatenate([wq[...], wk[...], wv[...], wg[...]], axis=1)
    proj = jnp.dot(rows, joined, preferred_element_type=F32)
    k_of, v_of = {}, {}
    for pi, (half, chunk) in enumerate(group):
        for j in range(2):
            r0 = (2 * pi + j) * ROWS
            block = proj[r0 : r0 + ROWS].astype(BF16)
            q = block[:, :HD].astype(F32)
            k = block[:, HD : 2 * HD].astype(F32)
            cs, sn = cos[chunk], sin[chunk]
            q = (q * cs + pltpu.roll(q, HD // 2, 1) * sn).astype(BF16)
            k = ((k * cs + pltpu.roll(k, HD // 2, 1) * sn) * HD ** (-0.5)).astype(BF16)
            qd = (q.astype(F32) * qdec[chunk]).astype(BF16)
            kd = (k.astype(F32) * kdec[chunk]).astype(BF16)
            v = block[:, 2 * HD : 3 * HD]
            out[pi, j, :, :HD] = q
            out[pi, j, :, HD : 2 * HD] = k
            out[pi, j, :, 2 * HD : 4 * HD] = block[:, 2 * HD :]
            out[pi, j, :, 4 * HD :] = qd
            k_of.setdefault(2 * half + j, []).append(kd)
            v_of.setdefault(2 * half + j, []).append(v)
    s_out = refs[-1] if last else refs[0]
    for s in range(4):
        kd = jnp.concatenate(k_of[s], axis=0)
        v = jnp.concatenate(v_of[s], axis=0)
        state = lax.dot_general(kd, v, (((0,), (0,)), ((), ())), preferred_element_type=F32)
        s_out[s] = state if first else s_in[s] + state
    if last:
        for d in range(4):
            refs[d][...] = s_out[lax.rem(idx[8] + d, 4)].astype(BF16)


def project(gi, pieces, weights, tables, s_in, idx):
    group = GROUPS[gi]
    n = len(group)
    first, last = s_in is None, gi == len(GROUPS) - 1
    ins = [*pieces, *weights, *tables]
    if last:
        ins = [idx, *ins]
    if not first:
        ins.append(s_in)
    outs = [sds((n, 2, ROWS, 5 * HD), BF16)]
    kernel = functools.partial(proj_kernel, group, first, last)
    if last:
        outs += [sds((HD, HD), BF16)] * 4
        scratch = [pltpu.VMEM((4, HD, HD), F32)]
    else:
        outs += [sds((4, HD, HD), F32)]
        scratch = []
    return pl.pallas_call(
        lambda *refs: kernel(refs),
        out_shape=outs,
        in_specs=[SM if last and i == 0 else VM for i in range(len(ins))],
        out_specs=[VM] * len(outs),
        scratch_shapes=scratch,
        cost_estimate=pl.CostEstimate(flops=n * 128 * 2048 * 512 * 2, bytes_accessed=1 << 20, transcendentals=0),
        name=f"proj{gi}",
    )(*ins)


def intra_kernel(*refs):
    held, (gap, gain, out, gate) = refs[:5], refs[5:]
    for s in range(4):

        def rows(lo, hi):
            parts = []
            for a in range(8):
                gi, pi, j = PLACE[(s, a)]
                parts.append(held[gi][pi, j, :, lo * HD : hi * HD])
            return jnp.concatenate(parts, axis=0)

        q, k, v = rows(0, 1), rows(1, 2), rows(2, 3)
        scores = lax.dot_general(q, k, (((1,), (1,)), ((), ())), preferred_element_type=F32)
        weights = (scores * gap[...]).astype(BF16)
        out[s] = jnp.dot(weights, v, preferred_element_type=F32)
        g = rows(3, 4).astype(F32)
        gate[s] = g * jax.nn.sigmoid(g) * gain[...]


def row_kernel(w, r0, r1, r2, r3, total):
    acc = None
    for d, r in enumerate((r0, r1, r2, r3)):
        term = r[...].astype(F32) * w[d]
        acc = term if acc is None else acc + term
    total[...] = acc.astype(BF16)


def z_kernel(w, t1, t2, t3, out):
    out[...] = (t1[...].astype(F32) + w[4] * t2[...].astype(F32) + w[5] * t3[...].astype(F32)).astype(BF16)


def carry_kernel(w, e0, e1, e2, r0, r1, r2, r3, c0, c1, c2, c3):
    before = e0[...].astype(F32) + w[6] * e1[...].astype(F32) + w[7] * e2[...].astype(F32)
    states = [r[...].astype(F32) for r in (r0, r1, r2, r3)]
    for d, c in enumerate((c0, c1, c2, c3)):
        acc = w[8 + 5 * d] * before
        for e in range(4):
            acc = acc + w[8 + 5 * d + 1 + e] * states[e]
        c[...] = acc.astype(BF16)


def read_kernel(*refs):
    idx, held, (part, gate) = refs[0], refs[1:6], refs[6:8]
    carries, outs, carry = refs[8:12], refs[12:20], refs[20]
    for d in range(4):
        carry[lax.rem(idx[8] + (4 - d), 4)] = carries[d][...]
    for s in range(4):
        parts = []
        for a in range(8):
            gi, pi, j = PLACE[(s, a)]
            parts.append(held[gi][pi, j, :, 4 * HD :])
        qd = jnp.concatenate(parts, axis=0)
        x = part[s] + jnp.dot(qd, carry[s], preferred_element_type=F32)
        x = x - jnp.mean(x, axis=-1, keepdims=True)
        var = jnp.mean(x * x, axis=-1, keepdims=True)
        y = (x * lax.rsqrt(var + group_eps) * gate[s]).astype(BF16)
        for a in range(8):
            outs[a][s] = y[a * ROWS : (a + 1) * ROWS]


def out_kernel(idx, *refs):
    pieces, (weight, gain, out) = refs[:8], refs[8:]
    acc = None
    north = idx[9] == 0
    for i in range(4):
        mine = pieces[2 * i][...].reshape(4 * ROWS, HD)
        other = pieces[2 * i + 1][...].reshape(4 * ROWS, HD)
        lhs = jnp.where(
            north, jnp.concatenate([mine, other], axis=1), jnp.concatenate([other, mine], axis=1)
        )
        row = pl.multiple_of(idx[10 + i] * 256, 256)
        term = jnp.dot(lhs, weight[pl.ds(row, 256), :], preferred_element_type=F32)
        acc = term if acc is None else acc + term
    scale = lax.rsqrt(jnp.mean(acc * acc, axis=-1, keepdims=True) + rms_eps)
    out[...] = (acc * scale * gain[...]).astype(BF16).reshape(out.shape)


def shift(value, axis, d, n):
    return lax.ppermute(value, axis, [(i, (i + d) % n) for i in range(n)])


def push(value, d):
    return lax.ppermute(value, "z", [(i, i + d) for i in range(NZ - d)])


def swap(value):
    return lax.ppermute(value, "c", [(0, 1), (1, 0)])


def exit_to(value, dx, dc):
    pairs = []
    for x in range(NX):
        for c in range(2):
            pairs.append((2 * x + c, 2 * ((x + dx) % NX) + (c ^ dc)))
    return lax.ppermute(value, ("x", "c"), pairs)


def body(tokens, in_gain, query_weight, key_weight, value_weight, gate_weight, log_decay, norm_gain, out_weight, post_gain):
    z, y, x, c = (lax.axis_index(a) for a in SP_TP)
    width = tokens.shape[-1]
    na, nb = call(
        norm_kernel, [sds((2, ROWS, width), BF16)] * 2, [tokens, in_gain.reshape(1, width)], 1 << 22, "norm"
    )
    left_a, right_b = shift(na, "x", 1, NX), shift(nb, "x", -1, NX)
    left_b, right_a = shift(nb, "x", 1, NX), shift(na, "x", -1, NX)
    far_a, far_b = shift(left_a, "x", 1, NX), shift(right_b, "x", -1, NX)

    xs = jnp.stack([x, (x + 3) % NX, (x + 1) % NX, (x + 2) % NX]).astype(jnp.int32)
    chunk_ids = (2 * xs[:, None] + jnp.stack([c, 1 - c])[None, :]).reshape(8)
    inner = (chunk_ids[:, None] * ROWS + jnp.arange(ROWS, dtype=jnp.int32)[None, :]).astype(jnp.int32)
    positions = ((z * NY + y) * STRETCH + inner).astype(F32)
    half = HD // 2
    lane = jnp.arange(HD, dtype=jnp.int32)
    inverse = rope_base ** (-(lane % half).astype(F32) / half)
    angles = positions[:, :, None] * inverse
    cos = jnp.cos(angles)
    sin = jnp.sin(angles) * jnp.where(lane < half, -1.0, 1.0)
    rate = log_decay[0]
    at = inner.astype(F32)
    qdec = jnp.broadcast_to(jnp.exp(rate * (at + 1.0))[:, :, None], (8, ROWS, HD))
    kdec = jnp.broadcast_to(jnp.exp(rate * (STRETCH - 1.0 - at))[:, :, None], (8, ROWS, HD))
    flat = at.reshape(STRETCH)
    apart = flat[:, None] - flat[None, :]
    gap = jnp.where(apart >= 0, jnp.exp(rate * jnp.maximum(apart, 0.0)), 0.0)
    idx = jnp.concatenate([chunk_ids, jnp.stack([y, c]), xs, jnp.zeros((2,), jnp.int32)]).astype(jnp.int32)
    src = (y - jnp.arange(4)) % 4
    dst = (y + jnp.arange(4)) % 4
    behind = dst[:, None] - 1 - src[None, :]
    carry_w = jnp.where(behind >= 0, jnp.exp(rate * STRETCH * jnp.maximum(behind, 0)), 0.0)
    row_span = STRETCH * NY
    scan_w = jnp.concatenate(
        [
            jnp.exp(rate * STRETCH * (3 - src)),
            jnp.exp(rate * row_span * jnp.array([1.0, 2.0, 3.0, 6.0], F32)),
            jnp.concatenate([jnp.exp(rate * STRETCH * dst)[:, None], carry_w], axis=1).reshape(20),
        ]
    ).astype(F32)

    weights = (query_weight, key_weight, value_weight, gate_weight)
    tables = (cos, sin, qdec, kdec)
    h0, s = project(0, (na, nb, swap(na), swap(nb)), weights, tables, None, None)
    h1, s = project(1, (left_a, right_b, swap(left_a), swap(right_b)), weights, tables, s, None)
    h2, s = project(2, (left_b, right_a, swap(left_b), swap(right_a)), weights, tables, s, None)
    h3, s = project(3, (far_a, far_b), weights, tables, s, None)
    h4, s0, s1, s2, s3 = project(4, (swap(far_a), swap(far_b)), weights, tables, s, idx)
    held = (h0, h1, h2, h3, h4)

    r1, r2, r3 = (shift(v, "y", d, NY) for d, v in ((1, s1), (2, s2), (3, s3)))
    state = sds((HD, HD), BF16)
    total = call(row_kernel, state, [scan_w, s0, r1, r2, r3], name="rows", smem=(0,))
    e0 = call(z_kernel, state, [scan_w, push(total, 1), push(total, 2), push(total, 3)], name="zsum", smem=(0,))
    c0, c1, c2, c3 = call(
        carry_kernel, [state] * 4, [scan_w, e0, push(e0, 3), push(e0, 6), s0, r1, r2, r3], name="carry", smem=(0,)
    )
    c1, c2, c3 = (shift(v, "y", d, NY) for d, v in ((1, c1), (2, c2), (3, c3)))

    part, gate = call(
        intra_kernel,
        [sds((4, STRETCH, HD), F32)] * 2,
        [*held, gap, norm_gain.reshape(1, HD)],
        4 * 4 * STRETCH * STRETCH * HD,
        "intra",
    )
    read_in = [idx, *held, part, gate, c0, c1, c2, c3]
    gated = pl.pallas_call(
        read_kernel,
        out_shape=[sds((4, ROWS, HD), BF16)] * 8,
        in_specs=[SM] + [VM] * (len(read_in) - 1),
        out_specs=[VM] * 8,
        scratch_shapes=[pltpu.VMEM((4, HD, HD), BF16)],
        cost_estimate=pl.CostEstimate(flops=1 << 28, bytes_accessed=1 << 20, transcendentals=0),
        name="read",
    )(*read_in)
    back = [
        gated[OWN],
        swap(gated[PART]),
        exit_to(gated[RIGHT], 1, 0),
        exit_to(gated[RIGHT_O], 1, 1),
        exit_to(gated[LEFT], -1, 0),
        exit_to(gated[LEFT_O], -1, 1),
        exit_to(gated[FAR], 2, 0),
        exit_to(gated[FAR_O], 2, 1),
    ]
    return call(
        out_kernel,
        sds(tokens.shape, BF16),
        [idx, *back, out_weight, post_gain.reshape(1, width)],
        256 * 1024 * 2048 * 2,
        "mix",
        smem=(0,),
    )


def solution(mesh):
    torus = Mesh(mesh.devices.reshape(NZ, NY, NX, 2), SP_TP)
    tp = ("x", "c")
    return jax.shard_map(
        body,
        mesh=torus,
        in_specs=(
            P(None, SP_TP, None),
            P(),
            P(None, tp),
            P(None, tp),
            P(None, tp),
            P(None, tp),
            P(tp),
            P(tp),
            P(),
            P(),
        ),
        out_specs=P(None, SP_TP, None),
        check_vma=False,
    )
```

```python
import functools

import jax
import jax.numpy as jnp
from jax import lax
from jax.experimental import pallas as pl
from jax.experimental.pallas import tpu as pltpu
from jax.sharding import Mesh
from jax.sharding import PartitionSpec as P


HD = 128
SP_TP = ("z", "y", "x", "c")
NX, NY, NZ = 4, 4, 8
ROWS = 64
STRETCH = 512
rms_eps = 1e-06
group_eps = 1e-05
rope_base = 10000.0
F32 = jnp.float32
BF16 = jnp.bfloat16

OWN, PART, LEFT, LEFT_O, RIGHT, RIGHT_O, FAR, FAR_O = range(8)
A, B = 0, 1
GROUPS = (
    ((A, OWN), (B, OWN), (A, PART), (B, PART)),
    ((A, LEFT), (B, RIGHT), (A, LEFT_O), (B, RIGHT_O)),
    ((B, LEFT), (A, RIGHT), (B, LEFT_O), (A, RIGHT_O)),
    ((A, FAR), (B, FAR)),
    ((A, FAR_O), (B, FAR_O)),
)
PLACE = {}
for gi, group in enumerate(GROUPS):
    for pi, (half, chunk) in enumerate(group):
        for j in range(2):
            PLACE[(2 * half + j, chunk)] = (gi, pi, j)

MIB = 1 << 20
VM = pl.BlockSpec(memory_space=pltpu.VMEM)
SM = pl.BlockSpec(memory_space=pltpu.SMEM)


def call(kernel, outs, ins, flops=0, name=None, smem=(), limit=2):
    specs = [SM if i in smem else VM for i in range(len(ins))]
    return pl.pallas_call(
        kernel,
        out_shape=outs,
        in_specs=specs,
        out_specs=jax.tree.map(lambda _: VM, outs),
        cost_estimate=pl.CostEstimate(flops=max(flops, 1), bytes_accessed=1 << 20, transcendentals=0),
        compiler_params=pltpu.CompilerParams(vmem_limit_bytes=limit * MIB),
        name=name,
    )(*ins)


def sds(shape, dtype):
    return jax.ShapeDtypeStruct(shape, dtype)


def norm_kernel(tok, gain, out):
    for s in range(2):
        x = tok[s].astype(F32)
        scale = lax.rsqrt(jnp.mean(x * x, axis=-1, keepdims=True) + rms_eps)
        out[s] = (x * scale * gain[...]).astype(BF16)


def normed_half(tokens, gain, half):
    width = tokens.shape[-1]
    block = (2, ROWS, width)
    return pl.pallas_call(
        norm_kernel,
        grid=(1,),
        out_shape=sds(block, BF16),
        in_specs=[pl.BlockSpec(block, lambda i: (half, 0, 0)), pl.BlockSpec((1, width), lambda i: (0, 0))],
        out_specs=pl.BlockSpec(block, lambda i: (0, 0, 0)),
        cost_estimate=pl.CostEstimate(flops=1 << 20, bytes_accessed=1 << 20, transcendentals=0),
        compiler_params=pltpu.CompilerParams(vmem_limit_bytes=8 * MIB),
        name=f"norm{half}",
    )(tokens, gain)


def proj_kernel(group, first, last, refs):
    n = len(group)
    pos = 0
    idx, refs = (refs[0], refs[1:]) if last else (None, refs)
    pieces, refs = refs[:n], refs[n:]
    wq, wk, wv, wg, cos, sin, qdec, kdec = refs[:8]
    refs = refs[8:]
    if not first:
        s_in, refs = refs[0], refs[1:]
    out, refs = refs[0], refs[1:]
    rows = jnp.concatenate([p[...].reshape(2 * ROWS, p.shape[-1]) for p in pieces], axis=0)
    joined = jnp.concatenate([wq[...], wk[...], wv[...], wg[...]], axis=1)
    proj = jnp.dot(rows, joined, preferred_element_type=F32)
    k_of, v_of = {}, {}
    for pi, (half, chunk) in enumerate(group):
        for j in range(2):
            r0 = (2 * pi + j) * ROWS
            block = proj[r0 : r0 + ROWS].astype(BF16)
            q = block[:, :HD].astype(F32)
            k = block[:, HD : 2 * HD].astype(F32)
            cs, sn = cos[chunk], sin[chunk]
            q = (q * cs + pltpu.roll(q, HD // 2, 1) * sn).astype(BF16)
            k = ((k * cs + pltpu.roll(k, HD // 2, 1) * sn) * HD ** (-0.5)).astype(BF16)
            qd = (q.astype(F32) * qdec[chunk]).astype(BF16)
            kd = (k.astype(F32) * kdec[chunk]).astype(BF16)
            v = block[:, 2 * HD : 3 * HD]
            out[pi, j, :, :HD] = q
            out[pi, j, :, HD : 2 * HD] = k
            out[pi, j, :, 2 * HD : 4 * HD] = block[:, 2 * HD :]
            out[pi, j, :, 4 * HD :] = qd
            k_of.setdefault(2 * half + j, []).append(kd)
            v_of.setdefault(2 * half + j, []).append(v)
    s_out = refs[-1] if last else refs[0]
    for s in range(4):
        kd = jnp.concatenate(k_of[s], axis=0)
        v = jnp.concatenate(v_of[s], axis=0)
        state = lax.dot_general(kd, v, (((0,), (0,)), ((), ())), preferred_element_type=F32)
        s_out[s] = state if first else s_in[s] + state
    if last:
        for d in range(4):
            refs[d][...] = s_out[lax.rem(idx[8] + d, 4)].astype(BF16)


def project(gi, pieces, weights, tables, s_in, idx):
    group = GROUPS[gi]
    n = len(group)
    first, last = s_in is None, gi == len(GROUPS) - 1
    ins = [*pieces, *weights, *tables]
    if last:
        ins = [idx, *ins]
    if not first:
        ins.append(s_in)
    outs = [sds((n, 2, ROWS, 5 * HD), BF16)]
    kernel = functools.partial(proj_kernel, group, first, last)
    if last:
        outs += [sds((HD, HD), BF16)] * 4
        scratch = [pltpu.VMEM((4, HD, HD), F32)]
    else:
        outs += [sds((4, HD, HD), F32)]
        scratch = []
    return pl.pallas_call(
        lambda *refs: kernel(refs),
        out_shape=outs,
        in_specs=[SM if last and i == 0 else VM for i in range(len(ins))],
        out_specs=[VM] * len(outs),
        scratch_shapes=scratch,
        cost_estimate=pl.CostEstimate(flops=n * 128 * 2048 * 512 * 2, bytes_accessed=1 << 20, transcendentals=0),
        compiler_params=pltpu.CompilerParams(vmem_limit_bytes=16 * MIB),
        name=f"proj{gi}",
    )(*ins)


def intra_kernel(*refs):
    held, (gap, gain, out, gate) = refs[:5], refs[5:]
    for s in range(4):

        def rows(lo, hi):
            parts = []
            for a in range(8):
                gi, pi, j = PLACE[(s, a)]
                parts.append(held[gi][pi, j, :, lo * HD : hi * HD])
            return jnp.concatenate(parts, axis=0)

        q, k, v = rows(0, 1), rows(1, 2), rows(2, 3)
        scores = lax.dot_general(q, k, (((1,), (1,)), ((), ())), preferred_element_type=F32)
        weights = (scores * gap[...]).astype(BF16)
        out[s] = jnp.dot(weights, v, preferred_element_type=F32)
        g = rows(3, 4).astype(F32)
        gate[s] = g * jax.nn.sigmoid(g) * gain[...]


def row_kernel(w, r0, r1, r2, r3, total):
    acc = None
    for d, r in enumerate((r0, r1, r2, r3)):
        term = r[...].astype(F32) * w[d]
        acc = term if acc is None else acc + term
    total[...] = acc.astype(BF16)


def z_kernel(w, t0, t1, out):
    out[...] = (t0[...].astype(F32) + w[4] * t1[...].astype(F32)).astype(BF16)


def carry_kernel(w, e0, e1, e2, e3, r0, r1, r2, r3, c0, c1, c2, c3):
    before = e0[...].astype(F32) + w[5] * e1[...].astype(F32) + w[6] * e2[...].astype(F32) + w[7] * e3[...].astype(F32)
    states = [r[...].astype(F32) for r in (r0, r1, r2, r3)]
    for d, c in enumerate((c0, c1, c2, c3)):
        acc = w[8 + 5 * d] * before
        for e in range(4):
            acc = acc + w[8 + 5 * d + 1 + e] * states[e]
        c[...] = acc.astype(BF16)


def read_kernel(*refs):
    idx, held, (part, gate) = refs[0], refs[1:6], refs[6:8]
    carries, outs, carry = refs[8:12], refs[12:20], refs[20]
    for d in range(4):
        carry[lax.rem(idx[8] + (4 - d), 4)] = carries[d][...]
    for s in range(4):
        parts = []
        for a in range(8):
            gi, pi, j = PLACE[(s, a)]
            parts.append(held[gi][pi, j, :, 4 * HD :])
        qd = jnp.concatenate(parts, axis=0)
        x = part[s] + jnp.dot(qd, carry[s], preferred_element_type=F32)
        x = x - jnp.mean(x, axis=-1, keepdims=True)
        var = jnp.mean(x * x, axis=-1, keepdims=True)
        y = (x * lax.rsqrt(var + group_eps) * gate[s]).astype(BF16)
        for a in range(8):
            outs[a][s] = y[a * ROWS : (a + 1) * ROWS]


def out_kernel(idx, *refs):
    pieces, (weight, gain, out) = refs[:8], refs[8:]
    acc = None
    north = idx[9] == 0
    for i in range(4):
        mine = pieces[2 * i][...].reshape(4 * ROWS, HD)
        other = pieces[2 * i + 1][...].reshape(4 * ROWS, HD)
        lhs = jnp.where(
            north, jnp.concatenate([mine, other], axis=1), jnp.concatenate([other, mine], axis=1)
        )
        row = pl.multiple_of(idx[10 + i] * 256, 256)
        term = jnp.dot(lhs, weight[pl.ds(row, 256), :], preferred_element_type=F32)
        acc = term if acc is None else acc + term
    scale = lax.rsqrt(jnp.mean(acc * acc, axis=-1, keepdims=True) + rms_eps)
    out[...] = (acc * scale * gain[...]).astype(BF16).reshape(out.shape)


def shift(value, axis, d, n):
    return lax.ppermute(value, axis, [(i, (i + d) % n) for i in range(n)])


def push(value, d):
    return lax.ppermute(value, "z", [(i, i + d) for i in range(NZ - d)])


def swap(value):
    return lax.ppermute(value, "c", [(0, 1), (1, 0)])


def exit_to(value, dx, dc):
    pairs = []
    for x in range(NX):
        for c in range(2):
            pairs.append((2 * x + c, 2 * ((x + dx) % NX) + (c ^ dc)))
    return lax.ppermute(value, ("x", "c"), pairs)


def body(tokens, in_gain, query_weight, key_weight, value_weight, gate_weight, log_decay, norm_gain, out_weight, post_gain):
    z, y, x, c = (lax.axis_index(a) for a in SP_TP)
    width = tokens.shape[-1]
    na, nb = (normed_half(tokens, in_gain.reshape(1, width), h) for h in (A, B))
    left_a, right_b = shift(na, "x", 1, NX), shift(nb, "x", -1, NX)
    left_b, right_a = shift(nb, "x", 1, NX), shift(na, "x", -1, NX)

    xs = jnp.stack([x, (x + 3) % NX, (x + 1) % NX, (x + 2) % NX]).astype(jnp.int32)
    chunk_ids = (2 * xs[:, None] + jnp.stack([c, 1 - c])[None, :]).reshape(8)
    inner = (chunk_ids[:, None] * ROWS + jnp.arange(ROWS, dtype=jnp.int32)[None, :]).astype(jnp.int32)
    positions = ((z * NY + y) * STRETCH + inner).astype(F32)
    half = HD // 2
    lane = jnp.arange(HD, dtype=jnp.int32)
    inverse = rope_base ** (-(lane % half).astype(F32) / half)
    angles = positions[:, :, None] * inverse
    cos = jnp.cos(angles)
    sin = jnp.sin(angles) * jnp.where(lane < half, -1.0, 1.0)
    rate = log_decay[0]
    at = inner.astype(F32)
    qdec = jnp.broadcast_to(jnp.exp(rate * (at + 1.0))[:, :, None], (8, ROWS, HD))
    kdec = jnp.broadcast_to(jnp.exp(rate * (STRETCH - 1.0 - at))[:, :, None], (8, ROWS, HD))
    flat = at.reshape(STRETCH)
    apart = flat[:, None] - flat[None, :]
    gap = jnp.where(apart >= 0, jnp.exp(rate * jnp.maximum(apart, 0.0)), 0.0)
    idx = jnp.concatenate([chunk_ids, jnp.stack([y, c]), xs, jnp.zeros((2,), jnp.int32)]).astype(jnp.int32)
    src = (y - jnp.arange(4)) % 4
    dst = (y + jnp.arange(4)) % 4
    behind = dst[:, None] - 1 - src[None, :]
    carry_w = jnp.where(behind >= 0, jnp.exp(rate * STRETCH * jnp.maximum(behind, 0)), 0.0)
    row_span = STRETCH * NY
    scan_w = jnp.concatenate(
        [
            jnp.exp(rate * STRETCH * (3 - src)),
            jnp.exp(rate * row_span * jnp.array([1.0, 2.0, 4.0, 6.0], F32)),
            jnp.concatenate([jnp.exp(rate * STRETCH * dst)[:, None], carry_w], axis=1).reshape(20),
        ]
    ).astype(F32)

    weights = (query_weight, key_weight, value_weight, gate_weight)
    tables = (cos, sin, qdec, kdec)
    h0, s = project(0, (na, nb, swap(na), swap(nb)), weights, tables, None, None)
    left_a, right_b, s = lax.optimization_barrier((left_a, right_b, s))
    far_a, far_b = shift(left_a, "x", 1, NX), shift(right_b, "x", -1, NX)
    h1, s = project(1, (left_a, right_b, swap(left_a), swap(right_b)), weights, tables, s, None)
    left_b, right_a, s = lax.optimization_barrier((left_b, right_a, s))
    h2, s = project(2, (left_b, right_a, swap(left_b), swap(right_a)), weights, tables, s, None)
    far_a, far_b, s = lax.optimization_barrier((far_a, far_b, s))
    h3, s = project(3, (far_a, far_b), weights, tables, s, None)
    h4, s0, s1, s2, s3 = project(4, (swap(far_a), swap(far_b)), weights, tables, s, idx)
    held = (h0, h1, h2, h3, h4)

    r1, r2, r3 = (shift(v, "y", d, NY) for d, v in ((1, s1), (2, s2), (3, s3)))
    state = sds((HD, HD), BF16)
    total = call(row_kernel, state, [scan_w, s0, r1, r2, r3], name="rows", smem=(0,))
    pair = call(z_kernel, state, [scan_w, total, push(total, 1)], name="zpair", smem=(0,))
    before = [push(pair, d) for d in (1, 3, 5, 7)]
    c0, c1, c2, c3 = call(
        carry_kernel, [state] * 4, [scan_w, *before, s0, r1, r2, r3], name="carry", smem=(0,)
    )
    c1, c2, c3 = (shift(v, "y", d, NY) for d, v in ((1, c1), (2, c2), (3, c3)))

    part, gate = call(
        intra_kernel,
        [sds((4, STRETCH, HD), F32)] * 2,
        [*held, gap, norm_gain.reshape(1, HD)],
        4 * 4 * STRETCH * STRETCH * HD,
        "intra",
        limit=20,
    )
    read_in = [idx, *held, part, gate, c0, c1, c2, c3]
    gated = pl.pallas_call(
        read_kernel,
        out_shape=[sds((4, ROWS, HD), BF16)] * 8,
        in_specs=[SM] + [VM] * (len(read_in) - 1),
        out_specs=[VM] * 8,
        scratch_shapes=[pltpu.VMEM((4, HD, HD), BF16)],
        cost_estimate=pl.CostEstimate(flops=1 << 28, bytes_accessed=1 << 20, transcendentals=0),
        compiler_params=pltpu.CompilerParams(vmem_limit_bytes=16 * MIB),
        name="read",
    )(*read_in)
    back = [
        gated[OWN],
        swap(gated[PART]),
        exit_to(gated[RIGHT], 1, 0),
        exit_to(gated[RIGHT_O], 1, 1),
        exit_to(gated[LEFT], -1, 0),
        exit_to(gated[LEFT_O], -1, 1),
        exit_to(gated[FAR], 2, 0),
        exit_to(gated[FAR_O], 2, 1),
    ]
    return call(
        out_kernel,
        sds(tokens.shape, BF16),
        [idx, *back, out_weight, post_gain.reshape(1, width)],
        256 * 1024 * 2048 * 2,
        "mix",
        smem=(0,),
        limit=20,
    )


def solution(mesh):
    torus = Mesh(mesh.devices.reshape(NZ, NY, NX, 2), SP_TP)
    tp = ("x", "c")
    return jax.shard_map(
        body,
        mesh=torus,
        in_specs=(
            P(None, SP_TP, None),
            P(),
            P(None, tp),
            P(None, tp),
            P(None, tp),
            P(None, tp),
            P(tp),
            P(tp),
            P(),
            P(),
        ),
        out_specs=P(None, SP_TP, None),
        check_vma=False,
    )
```

```python
import functools

import jax
import jax.numpy as jnp
from jax import lax
from jax.experimental import pallas as pl
from jax.experimental.pallas import tpu as pltpu
from jax.sharding import Mesh
from jax.sharding import PartitionSpec as P


HD = 128
SP_TP = ("z", "y", "x", "c")
NX, NY, NZ = 4, 4, 8
ROWS = 64
STRETCH = 512
rms_eps = 1e-06
group_eps = 1e-05
rope_base = 10000.0
F32 = jnp.float32
BF16 = jnp.bfloat16

OWN, PART, LEFT, LEFT_O, RIGHT, RIGHT_O, FAR, FAR_O = range(8)
A, B = 0, 1
GROUPS = (
    ((A, OWN), (B, OWN), (A, PART), (B, PART)),
    ((A, LEFT), (B, RIGHT), (A, LEFT_O), (B, RIGHT_O)),
    ((B, LEFT), (A, RIGHT), (B, LEFT_O), (A, RIGHT_O)),
    ((A, FAR), (B, FAR)),
    ((A, FAR_O), (B, FAR_O)),
)
PLACE = {}
for gi, group in enumerate(GROUPS):
    for pi, (half, chunk) in enumerate(group):
        for j in range(2):
            PLACE[(2 * half + j, chunk)] = (gi, pi, j)

MIB = 1 << 20
VM = pl.BlockSpec(memory_space=pltpu.VMEM)
SM = pl.BlockSpec(memory_space=pltpu.SMEM)
HB = pl.BlockSpec(memory_space=pltpu.HBM)
AN = pl.BlockSpec(memory_space=pl.ANY)


def call(kernel, outs, ins, flops=0, smem=(), limit=2, keep=(), scratch=()):
    specs = [SM if i in smem else VM for i in range(len(ins))] + [AN] * len(keep)
    n = len(ins)

    def run(*refs):
        kernel(*refs[:n], *refs[n + len(keep) :])

    return pl.pallas_call(
        run,
        out_shape=outs,
        in_specs=specs,
        out_specs=jax.tree.map(lambda _: VM, outs),
        scratch_shapes=list(scratch),
        cost_estimate=pl.CostEstimate(flops=max(flops, 1), bytes_accessed=1 << 20, transcendentals=0),
        compiler_params=pltpu.CompilerParams(vmem_limit_bytes=limit * MIB),
    )(*ins, *keep)


def sds(shape, dtype):
    return jax.ShapeDtypeStruct(shape, dtype)


def norm_kernel(half, tok, gain, out, rows, scale_row, sems):
    copies = [pltpu.make_async_copy(gain, scale_row, sems.at[2])]
    for s in range(2):
        copies.append(pltpu.make_async_copy(tok.at[2 * half + s], rows.at[s], sems.at[s]))
    for copy in copies:
        copy.start()
    for s in range(2):
        copies[1 + s].wait()
        if s == 0:
            copies[0].wait()
        x = rows[s].astype(F32)
        scale = lax.rsqrt(jnp.mean(x * x, axis=-1, keepdims=True) + rms_eps)
        out[s] = (x * scale * scale_row[...]).astype(BF16)


def normed_half(tokens, gain, half):
    width = tokens.shape[-1]
    block = (2, ROWS, width)
    return pl.pallas_call(
        functools.partial(norm_kernel, half),
        out_shape=sds(block, BF16),
        in_specs=[HB, HB],
        out_specs=VM,
        scratch_shapes=[
            pltpu.VMEM(block, BF16),
            pltpu.VMEM((1, width), F32),
            pltpu.SemaphoreType.DMA((3,)),
        ],
        cost_estimate=pl.CostEstimate(flops=1 << 20, bytes_accessed=1 << 20, transcendentals=0),
        compiler_params=pltpu.CompilerParams(vmem_limit_bytes=8 * MIB),
    )(tokens, gain)


def proj_kernel(group, first, last, refs):
    n = len(group)
    idx, refs = (refs[0], refs[1:]) if last else (None, refs)
    pieces, refs = refs[:n], refs[n:]
    wq, wk, wv, wg, cos, sin, qdec, kdec = refs[:8]
    refs = refs[8:]
    if not first:
        s_in, refs = refs[0], refs[1:]
    out, refs = refs[0], refs[1:]
    rows = jnp.concatenate([p[...].reshape(2 * ROWS, p.shape[-1]) for p in pieces], axis=0)
    joined = jnp.concatenate([wq[...], wk[...], wv[...], wg[...]], axis=1)
    proj = jnp.dot(rows, joined, preferred_element_type=F32)
    k_of, v_of = {}, {}
    for pi, (half, chunk) in enumerate(group):
        for j in range(2):
            r0 = (2 * pi + j) * ROWS
            block = proj[r0 : r0 + ROWS].astype(BF16)
            q = block[:, :HD].astype(F32)
            k = block[:, HD : 2 * HD].astype(F32)
            cs, sn = cos[chunk], sin[chunk]
            q = (q * cs + pltpu.roll(q, HD // 2, 1) * sn).astype(BF16)
            k = ((k * cs + pltpu.roll(k, HD // 2, 1) * sn) * HD ** (-0.5)).astype(BF16)
            qd = (q.astype(F32) * qdec[chunk]).astype(BF16)
            kd = (k.astype(F32) * kdec[chunk]).astype(BF16)
            v = block[:, 2 * HD : 3 * HD]
            out[pi, j, :, :HD] = q
            out[pi, j, :, HD : 2 * HD] = k
            out[pi, j, :, 2 * HD : 4 * HD] = block[:, 2 * HD :]
            out[pi, j, :, 4 * HD :] = qd
            k_of.setdefault(2 * half + j, []).append(kd)
            v_of.setdefault(2 * half + j, []).append(v)
    s_out = refs[-1] if last else refs[0]
    for s in range(4):
        kd = jnp.concatenate(k_of[s], axis=0)
        v = jnp.concatenate(v_of[s], axis=0)
        state = lax.dot_general(kd, v, (((0,), (0,)), ((), ())), preferred_element_type=F32)
        s_out[s] = state if first else s_in[s] + state
    if last:
        for d in range(4):
            refs[d][...] = s_out[lax.rem(idx[8] + d, 4)].astype(BF16)


def project(gi, pieces, weights, tables, s_in, idx, keep):
    group = GROUPS[gi]
    n = len(group)
    first, last = s_in is None, gi == len(GROUPS) - 1
    ins = [*pieces, *weights, *tables]
    if last:
        ins = [idx, *ins]
    if not first:
        ins.append(s_in)
    outs = [sds((n, 2, ROWS, 5 * HD), BF16)]
    if last:
        outs += [sds((HD, HD), BF16)] * 4
        scratch = [pltpu.VMEM((4, HD, HD), F32)]
    else:
        outs += [sds((4, HD, HD), F32)]
        scratch = []
    kernel = functools.partial(proj_kernel, group, first, last)
    return call(
        lambda *refs: kernel(refs),
        outs,
        ins,
        n * 128 * 2048 * 512 * 2,
        smem=(0,) if last else (),
        limit=12,
        keep=keep,
        scratch=scratch,
    )


def intra_kernel(*refs):
    held, (gap, gain, out, gate) = refs[:5], refs[5:]
    for s in range(4):

        def rows(lo, hi):
            parts = []
            for a in range(8):
                gi, pi, j = PLACE[(s, a)]
                parts.append(held[gi][pi, j, :, lo * HD : hi * HD])
            return jnp.concatenate(parts, axis=0)

        q, k, v = rows(0, 1), rows(1, 2), rows(2, 3)
        scores = lax.dot_general(q, k, (((1,), (1,)), ((), ())), preferred_element_type=F32)
        weights = (scores * gap[...]).astype(BF16)
        out[s] = jnp.dot(weights, v, preferred_element_type=F32)
        g = rows(3, 4).astype(F32)
        gate[s] = g * jax.nn.sigmoid(g) * gain[...]


def row_kernel(w, r0, r1, r2, r3, total):
    acc = None
    for d, r in enumerate((r0, r1, r2, r3)):
        term = r[...].astype(F32) * w[d]
        acc = term if acc is None else acc + term
    total[...] = acc.astype(BF16)


def pair_kernel(w, step, mine, theirs, before, total_out, before_out):
    a, b = mine[...].astype(F32), theirs[...].astype(F32)
    total_out[...] = (w[4 + 3 * step] * a + w[5 + 3 * step] * b).astype(BF16)
    old = 0.0 if before is None else before[...]
    before_out[...] = old + w[6 + 3 * step] * b


def first_pair(w, mine, theirs, total_out, before_out):
    pair_kernel(w, 0, mine, theirs, None, total_out, before_out)


def second_pair(w, mine, theirs, before, total_out, before_out):
    pair_kernel(w, 1, mine, theirs, before, total_out, before_out)


def carry_kernel(w, theirs, before_in, r0, r1, r2, r3, c0, c1, c2, c3):
    before = before_in[...] + w[10] * theirs[...].astype(F32)
    states = [r[...].astype(F32) for r in (r0, r1, r2, r3)]
    for d, c in enumerate((c0, c1, c2, c3)):
        acc = w[11 + 5 * d] * before
        for e in range(4):
            acc = acc + w[12 + 5 * d + e] * states[e]
        c[...] = acc.astype(BF16)


def read_kernel(*refs):
    idx, held, (part, gate) = refs[0], refs[1:6], refs[6:8]
    carries, outs, carry = refs[8:12], refs[12:16], refs[16]
    for d in range(4):
        carry[lax.rem(idx[8] + (4 - d), 4)] = carries[d][...]
    for s in range(4):
        parts = []
        for a in range(8):
            gi, pi, j = PLACE[(s, a)]
            parts.append(held[gi][pi, j, :, 4 * HD :])
        qd = jnp.concatenate(parts, axis=0)
        x = part[s] + jnp.dot(qd, carry[s], preferred_element_type=F32)
        x = x - jnp.mean(x, axis=-1, keepdims=True)
        var = jnp.mean(x * x, axis=-1, keepdims=True)
        y = (x * lax.rsqrt(var + group_eps) * gate[s]).astype(BF16)
        for a in range(8):
            outs[a // 2][a % 2, s] = y[a * ROWS : (a + 1) * ROWS]


def out_kernel(idx, *refs):
    mine, others, (weight, gain, out) = refs[:4], refs[4:8], refs[8:]
    acc = None
    north = idx[9] == 0
    for i in range(4):
        one = mine[i][0].reshape(4 * ROWS, HD)
        two = others[i][1].reshape(4 * ROWS, HD)
        lhs = jnp.where(north, jnp.concatenate([one, two], axis=1), jnp.concatenate([two, one], axis=1))
        row = pl.multiple_of(idx[10 + i] * 256, 256)
        term = jnp.dot(lhs, weight[pl.ds(row, 256), :], preferred_element_type=F32)
        acc = term if acc is None else acc + term
    scale = lax.rsqrt(jnp.mean(acc * acc, axis=-1, keepdims=True) + rms_eps)
    out[...] = (acc * scale * gain[...]).astype(BF16).reshape(out.shape)


def shift(value, axis, d, n):
    return lax.ppermute(value, axis, [(i, (i + d) % n) for i in range(n)])


def pairs_z(value, mask):
    return lax.ppermute(value, "z", [(i, i ^ mask) for i in range(NZ)])


def swap(value):
    return lax.ppermute(value, "c", [(0, 1), (1, 0)])


def body(tokens, in_gain, query_weight, key_weight, value_weight, gate_weight, log_decay, norm_gain, out_weight, post_gain):
    z, y, x, c = (lax.axis_index(a) for a in SP_TP)
    width = tokens.shape[-1]
    na, nb = (normed_half(tokens, in_gain.reshape(1, width), h) for h in (A, B))
    left_a, right_b = shift(na, "x", 1, NX), shift(nb, "x", -1, NX)
    left_b, right_a = shift(nb, "x", 1, NX), shift(na, "x", -1, NX)
    far_a, far_b = shift(left_a, "x", 1, NX), shift(right_b, "x", -1, NX)

    xs = jnp.stack([x, (x + 3) % NX, (x + 1) % NX, (x + 2) % NX]).astype(jnp.int32)
    chunk_ids = (2 * xs[:, None] + jnp.stack([c, 1 - c])[None, :]).reshape(8)
    inner = (chunk_ids[:, None] * ROWS + jnp.arange(ROWS, dtype=jnp.int32)[None, :]).astype(jnp.int32)
    positions = ((z * NY + y) * STRETCH + inner).astype(F32)
    half = HD // 2
    lane = jnp.arange(HD, dtype=jnp.int32)
    inverse = rope_base ** (-(lane % half).astype(F32) / half)
    angles = positions[:, :, None] * inverse
    cos = jnp.cos(angles)
    sin = jnp.sin(angles) * jnp.where(lane < half, -1.0, 1.0)
    rate = log_decay[0]
    at = inner.astype(F32)
    qdec = jnp.broadcast_to(jnp.exp(rate * (at + 1.0))[:, :, None], (8, ROWS, HD))
    kdec = jnp.broadcast_to(jnp.exp(rate * (STRETCH - 1.0 - at))[:, :, None], (8, ROWS, HD))
    flat = at.reshape(STRETCH)
    apart = flat[:, None] - flat[None, :]
    gap = jnp.where(apart >= 0, jnp.exp(rate * jnp.maximum(apart, 0.0)), 0.0)
    idx = jnp.concatenate([chunk_ids, jnp.stack([y, c]), xs, jnp.zeros((2,), jnp.int32)]).astype(jnp.int32)
    src = (y - jnp.arange(4)) % 4
    dst = (y + jnp.arange(4)) % 4
    behind = dst[:, None] - 1 - src[None, :]
    carry_w = jnp.where(behind >= 0, jnp.exp(rate * STRETCH * jnp.maximum(behind, 0)), 0.0)
    span = rate * STRETCH * NY
    b0, b1, b2 = z % 2, (z // 2) % 2, z // 4
    zero = jnp.zeros((), F32)
    one = jnp.ones((), F32)

    def when(bit, yes, no):
        return jnp.where(bit == 1, yes, no)

    steps = jnp.stack(
        [
            when(b0, one, jnp.exp(span)),
            when(b0, jnp.exp(span), one),
            when(b0, one, zero),
            when(b1, one, jnp.exp(2 * span)),
            when(b1, jnp.exp(2 * span), one),
            when(b1, jnp.exp(span * b0), zero),
            when(b2, jnp.exp(span * (z % 4)), zero),
        ]
    )
    scan_w = jnp.concatenate(
        [
            jnp.exp(rate * STRETCH * (3 - src)),
            steps,
            jnp.concatenate([jnp.exp(rate * STRETCH * dst)[:, None], carry_w], axis=1).reshape(20),
            jnp.zeros((1,), F32),
        ]
    ).astype(F32)

    weights = (query_weight, key_weight, value_weight, gate_weight)
    tables = (cos, sin, qdec, kdec)
    h0, s = project(0, (na, nb, swap(na), swap(nb)), weights, tables, None, None, ())
    h1, s = project(1, (left_a, right_b, swap(left_a), swap(right_b)), weights, tables, s, None, (h0,))
    h2, s = project(2, (left_b, right_a, swap(left_b), swap(right_a)), weights, tables, s, None, (h0, h1))
    h3, s = project(3, (far_a, far_b), weights, tables, s, None, (h0, h1, h2))
    swapped = [swap(v) for v in (far_a, far_b)]
    h4, s0, s1, s2, s3 = project(4, swapped, weights, tables, s, idx, (h0, h1, h2, h3))
    held = (h0, h1, h2, h3, h4)

    r1, r2, r3 = (shift(v, "y", d, NY) for d, v in ((1, s1), (2, s2), (3, s3)))
    state, wide = sds((HD, HD), BF16), sds((HD, HD), F32)
    total = call(row_kernel, state, [scan_w, s0, r1, r2, r3], smem=(0,), keep=held)
    total, before = call(first_pair, [state, wide], [scan_w, total, pairs_z(total, 1)], smem=(0,), keep=held)
    total, before = call(second_pair, [state, wide], [scan_w, total, pairs_z(total, 2), before], smem=(0,), keep=held)
    c0, c1, c2, c3 = call(
        carry_kernel, [state] * 4, [scan_w, pairs_z(total, 7), before, s0, r1, r2, r3], smem=(0,), keep=held
    )
    c1, c2, c3 = (shift(v, "y", d, NY) for d, v in ((1, c1), (2, c2), (3, c3)))

    part, gate = call(
        intra_kernel,
        [sds((4, STRETCH, HD), F32)] * 2,
        [*held, gap, norm_gain.reshape(1, HD)],
        4 * 4 * STRETCH * STRETCH * HD,
        limit=16,
    )
    g_own, g_left, g_right, g_far = call(
        read_kernel,
        [sds((2, 4, ROWS, HD), BF16)] * 4,
        [idx, *held, part, gate, c0, c1, c2, c3],
        1 << 28,
        smem=(0,),
        limit=16,
        scratch=[pltpu.VMEM((4, HD, HD), BF16)],
    )
    mine = [g_own, shift(g_right, "x", 1, NX), shift(g_left, "x", -1, NX), shift(g_far, "x", 2, NX)]
    others = [swap(v) for v in mine]
    return call(
        out_kernel,
        sds(tokens.shape, BF16),
        [idx, *mine, *others, out_weight, post_gain.reshape(1, width)],
        256 * 1024 * 2048 * 2,
        smem=(0,),
        limit=16,
    )


def solution(mesh):
    torus = Mesh(mesh.devices.reshape(NZ, NY, NX, 2), SP_TP)
    tp = ("x", "c")
    return jax.shard_map(
        body,
        mesh=torus,
        in_specs=(
            P(None, SP_TP, None),
            P(),
            P(None, tp),
            P(None, tp),
            P(None, tp),
            P(None, tp),
            P(tp),
            P(tp),
            P(),
            P(),
        ),
        out_specs=P(None, SP_TP, None),
        check_vma=False,
    )
```
